32 devices in a mesh: sp: 16 (over z, y, x), tp: 2 (over core).
Axes of the slice: x: 2, y: 2, z: 4, core: 2. Of those that a mesh axis runs over, the one named last changes fastest.
Arguments:
- block_input: bfloat16 [1, 1024, 4096], P(None, 'sp', 'tp'), may hold values from -6 to 6
- key_weight: bfloat16 [4096, 2048], P('sp', 'tp'), may hold values from -0.09375 to 0.09375
- value_weight: bfloat16 [4096, 2048], P('sp', 'tp'), may hold values from -0.09375 to 0.09375
- earlier_keys: bfloat16 [1, 4096, 2048], P(None, 'sp', 'tp'), may hold values from -10 to 10
- past_values: bfloat16 [1, 4096, 2048], P(None, 'sp', 'tp'), may hold values from -6 to 6
- past_gates: float32 [1, 16, 4096], P(None, 'tp', 'sp'), may hold values from -770.15 to 0, as said below
- block_gates: float32 [1, 16, 1024], P(None, 'tp', 'sp'), may hold values from -770.15 to 0
- step_query: bfloat16 [1, 2048], P(None, 'tp'), may hold values from -12 to 12
- step_key: bfloat16 [1, 2048], P(None, 'tp'), may hold values from -10 to 10
- step_value: bfloat16 [1, 2048], P(None, 'tp'), may hold values from -6 to 6
- step_gate: float32 [1, 16], P(None, 'tp'), may hold values from -770.15 to 0, as said below
Outputs:
- cache_keys: bfloat16 [16, 320, 2048], P('sp', None, 'tp')
- stored_vector_entries: bfloat16 [16, 320, 2048], P('sp', None, 'tp')
- cache_gates: float32 [16, 16, 320], P('sp', 'tp')
- initial_attention_output: float32 [1, 2048], P(None, 'tp')
The draws below stay inside these ranges and needn't reach their ends.
Inputs may be any that keep to these rules, and one draw needn't show every extreme that they name: Cumulative sums of negative log gates along each sequence and head; they never rise from one position to the next, and block_gates continue past_gates. `step_gate`: the cumulative log gate one position after the block, no larger than the block's last.
All inputs are finite; a program needn't handle non-finite values.
Results may differ from the reference program's by a relative error of at most 0.0055.
Values may be sent and summed in bfloat16 or wider, within the bound.
A program may use at most 64 MiB of HBM per device.

```python
import jax
import jax.numpy as jnp
from jax import lax

D = 4096
HEADS = 16
HEAD_DIM = 128
GROUP = 16
SPAN = 64
PAST_SPAN = 256
SEQS = 1
BLOCK_LEN = 1024
PAST_LEN = 4096
N_SP = 16


def rank_heads(subkey):
    return jax.random.permutation(subkey, HEADS)


def chain_gates(key):
    chain_len = PAST_LEN + BLOCK_LEN + 1
    positions = jnp.arange(chain_len, dtype=jnp.int32)
    device_of = jnp.where(positions < PAST_LEN, positions // PAST_SPAN, (positions - PAST_LEN) // SPAN)
    device_of = jnp.minimum(device_of, N_SP - 1)
    keys_all = jax.random.split(jax.random.fold_in(key, 101), 7)
    head_ranks = jax.vmap(rank_heads)(jax.random.split(keys_all[0], SEQS))
    rapid_attention_pick = head_ranks < HEADS // 2
    slow_total = jax.random.uniform(keys_all[1], (SEQS, HEADS), jnp.float32, 0.2, 0.8)
    fast_reach = jax.random.uniform(keys_all[2], (SEQS, HEADS), jnp.float32, 30.0, 100.0)
    base_rate = jnp.where(rapid_attention_pick, 1.0 / fast_reach, slow_total / chain_len)
    device_scale = jnp.exp(jax.random.uniform(keys_all[3], (SEQS, N_SP), jnp.float32, -0.7, 0.7))
    rough = jnp.exp(jax.random.uniform(keys_all[4], (SEQS, HEADS, chain_len), jnp.float32, -0.7, 0.7))
    forgetting_factor_each_move = base_rate[:, :, None] * device_scale[:, device_of][:, None, :] * rough
    spots = jax.random.randint(keys_all[5], (SEQS, HEADS, 3), 0, chain_len)
    layer_count_overall = jax.random.uniform(keys_all[6], (SEQS, HEADS, 3), jnp.float32, 0.22, 0.45)
    agreement_count = positions[None, None, None, :] == spots[:, :, :, None]
    decoded_item_count = jnp.sum(jnp.where(agreement_count, layer_count_overall[:, :, :, None], 0.0), axis=2)
    decoded_item_count = decoded_item_count * jnp.where(rapid_attention_pick, 0.0, 1.0)[:, :, None]
    return jnp.cumsum(-(forgetting_factor_each_move + decoded_item_count), axis=2)


def draw_past_gates(key, part):
    return chain_gates(key)[:, :, :PAST_LEN]


def draw_block_gates(key, part):
    return chain_gates(key)[:, :, PAST_LEN:PAST_LEN + BLOCK_LEN]


def draw_step_gate(key, part):
    return chain_gates(key)[:, :, PAST_LEN + BLOCK_LEN]


def draw_earlier_keys(key, part):
    normal_rows = jax.random.normal(jax.random.fold_in(key, 303), (SEQS, PAST_LEN, HEADS * HEAD_DIM), jnp.float32)
    normal_rows = jnp.clip(normal_rows, -6.0, 6.0)
    return normal_rows.astype(jnp.bfloat16)


def draw_step_query(key, part):
    result = jnp.clip(3.0 * jax.random.normal(jax.random.fold_in(key, 404), (SEQS, HEADS * HEAD_DIM), jnp.float32), -12.0, 12.0)
    return result.astype(jnp.bfloat16)


def draw_step_key(key, part):
    result = jnp.clip(2.5 * jax.random.normal(jax.random.fold_in(key, 505), (SEQS, HEADS * HEAD_DIM), jnp.float32), -10.0, 10.0)
    return result.astype(jnp.bfloat16)


def steps_of(key, shape, shards, smallest, largest):
    loudness = 1.0
    for dim, blocks in shards:
        draws = jax.random.uniform(jax.random.fold_in(jax.random.fold_in(key, 6), dim), (blocks,), jnp.float32, smallest / len(shards), largest / len(shards))
        loudness = loudness * jnp.repeat(jnp.exp(draws), shape[dim] // blocks).reshape((-1,) + (1,) * (len(shape) - 1 - dim))
    return loudness


def noise(key, dims, width, reach, cuts=(), held_as=jnp.bfloat16):
    level = steps_of(key, dims, cuts, -0.22, 0.18) if cuts else 1.0
    values = jax.random.normal(key, dims, jnp.float32) * width * level
    return jnp.minimum(jnp.maximum(values, -reach), reach).astype(held_as)


def setup_inputs(seed: int = 0) -> dict:
    splits = jax.random.split(jax.random.key(seed), 12)
    return {
        "block_input": noise(splits[0], (SEQS, BLOCK_LEN, D), 1.0, 6.0, ((1, 16), (2, 2))),
        "key_weight": noise(splits[1], (D, HEADS * HEAD_DIM), D ** -0.5, 0.09375, ((0, 16), (1, 2))),
        "value_weight": noise(splits[2], (D, HEADS * HEAD_DIM), D ** -0.5, 0.09375, ((0, 16), (1, 2))),
        "earlier_keys": draw_earlier_keys(jax.random.fold_in(splits[11], 71), 0),
        "past_values": noise(splits[4], (SEQS, PAST_LEN, HEADS * HEAD_DIM), 1.0, 6.0, ((1, 16), (2, 2))),
        "past_gates": draw_past_gates(jax.random.fold_in(splits[11], 71), 0),
        "block_gates": draw_block_gates(jax.random.fold_in(splits[11], 71), 0),
        "step_query": draw_step_query(jax.random.fold_in(splits[11], 71), 0),
        "step_key": draw_step_key(jax.random.fold_in(splits[11], 71), 0),
        "step_value": noise(splits[9], (SEQS, HEADS * HEAD_DIM), 1.0, 6.0, ((1, 2),)),
        "step_gate": draw_step_gate(jax.random.fold_in(splits[11], 71), 0),
    }


def relayout_rows(past_rows, block_rows):
    sequences = past_rows.shape[0]
    row_width = past_rows.shape[2]
    past_parts = past_rows.reshape(sequences, N_SP, GROUP, PAST_SPAN // GROUP, row_width)
    block_parts = block_rows.reshape(sequences, N_SP, GROUP, SPAN // GROUP, row_width)
    joined = jnp.concatenate([past_parts, block_parts], axis=3)
    joined = joined.transpose(0, 2, 1, 3, 4)
    return joined.reshape(sequences * GROUP, -1, row_width)


def relayout_gates(past_gates, block_gates):
    sequences = past_gates.shape[0]
    head_count = past_gates.shape[1]
    past_parts = past_gates.reshape(sequences, head_count, N_SP, GROUP, PAST_SPAN // GROUP)
    block_parts = block_gates.reshape(sequences, head_count, N_SP, GROUP, SPAN // GROUP)
    joined = jnp.concatenate([past_parts, block_parts], axis=4)
    joined = joined.transpose(0, 3, 1, 2, 4)
    return joined.reshape(sequences * GROUP, head_count, -1)


def read_sequence(operands):
    queries, past_key, block_key, past_value, block_value, past_gate, block_gate, own_key, own_value, own_gate = operands
    scale = HEAD_DIM ** -0.5

    def read_head(head):
        offset = head * HEAD_DIM
        query_head = lax.dynamic_slice_in_dim(queries, offset, HEAD_DIM, 0).astype(jnp.float32)
        key_rows = jnp.concatenate([lax.dynamic_slice_in_dim(past_key, offset, HEAD_DIM, 1),
                                    lax.dynamic_slice_in_dim(block_key, offset, HEAD_DIM, 1)], axis=0).astype(jnp.float32)
        value_rows = jnp.concatenate([lax.dynamic_slice_in_dim(past_value, offset, HEAD_DIM, 1),
                                      lax.dynamic_slice_in_dim(block_value, offset, HEAD_DIM, 1)], axis=0).astype(jnp.float32)
        gate_rows = jnp.concatenate([lax.dynamic_index_in_dim(past_gate, head, 0, keepdims=False),
                                     lax.dynamic_index_in_dim(block_gate, head, 0, keepdims=False)], axis=0)
        gate_here = lax.dynamic_index_in_dim(own_gate, head, 0, keepdims=False)
        own_key_head = lax.dynamic_slice_in_dim(own_key, offset, HEAD_DIM, 0).astype(jnp.float32)
        own_value_head = lax.dynamic_slice_in_dim(own_value, offset, HEAD_DIM, 0).astype(jnp.float32)
        scores = jnp.dot(key_rows, query_head, precision=lax.Precision.HIGHEST) * scale + gate_here - gate_rows
        own_score = jnp.dot(own_key_head, query_head, precision=lax.Precision.HIGHEST) * scale
        maximum = jnp.maximum(jnp.max(scores), own_score)
        weights = jnp.exp(scores - maximum)
        own_weight = jnp.exp(own_score - maximum)
        denominator = jnp.sum(weights) + own_weight
        summed = jnp.dot(weights, value_rows, precision=lax.Precision.HIGHEST) + own_weight * own_value_head
        return summed / denominator

    return lax.map(read_head, jnp.arange(HEADS, dtype=jnp.int32)).reshape(-1)


def reference(block_input, key_weight, value_weight, earlier_keys, past_values, past_gates, block_gates, step_query, step_key, step_value, step_gate):
    sequences = block_input.shape[0]
    flat_input = block_input.reshape(-1, block_input.shape[2])
    block_keys = jnp.dot(flat_input, key_weight, preferred_element_type=jnp.float32).astype(jnp.bfloat16)
    block_keys = block_keys.reshape(sequences, -1, key_weight.shape[1])
    block_values = jnp.dot(flat_input, value_weight, preferred_element_type=jnp.float32).astype(jnp.bfloat16)
    block_values = block_values.reshape(sequences, -1, value_weight.shape[1])
    cache_keys = relayout_rows(earlier_keys, block_keys)
    stored_vector_entries = relayout_rows(past_values, block_values)
    cache_gates = relayout_gates(past_gates, block_gates)
    initial_attention_output = lax.map(read_sequence, (step_query, earlier_keys, block_keys, past_values, block_values,
                                        past_gates, block_gates, step_key, step_value, step_gate))
    return cache_keys, stored_vector_entries, cache_gates, initial_attention_output
```

```python
import functools

import jax
import jax.numpy as jnp
from jax import lax
from jax.experimental import pallas as pl
from jax.experimental.pallas import tpu as pltpu
from jax.sharding import PartitionSpec as P

HEAD_DIM = 128
GROUP = 16


lowest_score_bound = -1e30


def merged_2(part, axis, combine):
    gathered = jax.tree.map(lambda a: lax.all_gather(a, axis), part)

    def take(source):
        return jax.tree.map(lambda a: lax.dynamic_index_in_dim(a, source, 0, False), gathered)

    return lax.fori_loop(
        1, lax.axis_size(axis), lambda source, state: combine(state, take(source)), take(0)
    )


def share_split(source_rows, shares):
    return source_rows.reshape(shares, -1, source_rows.shape[2])


def partial_read(queries, key_rows, value_rows, gate_rows, gate_here):
    sequences, row_count = (key_rows.shape[0], key_rows.shape[1])
    local_heads, head_width = (queries.shape[1], queries.shape[2])
    key_rows = key_rows.reshape(sequences, row_count, local_heads, head_width)
    value_rows = value_rows.reshape(sequences, row_count, local_heads, head_width)
    scores = jnp.einsum("shd,srhd->shr", queries, key_rows, preferred_element_type=jnp.float32)
    scores = scores * head_width ** (-0.5) + gate_here[:, :, None] - gate_rows
    maximum = jnp.max(scores, axis=2)
    weights = jnp.exp(scores - maximum[:, :, None])
    denominator = jnp.sum(weights, axis=2)
    summed = jnp.einsum(
        "shr,srhd->shd", weights, value_rows.astype(jnp.float32), precision=lax.Precision.HIGHEST
    )
    return (maximum, denominator, summed)


def combine_reads(former, latter):
    maximum = jnp.maximum(former[0], latter[0])
    former_scale = jnp.exp(former[0] - maximum)
    latter_scale = jnp.exp(latter[0] - maximum)
    return (
        maximum,
        former[1] * former_scale + latter[1] * latter_scale,
        former[2] * former_scale[:, :, None] + latter[2] * latter_scale[:, :, None],
    )


def local(
    block_input,
    key_weight,
    value_weight,
    earlier_keys,
    past_values,
    past_gates,
    block_gates,
    step_query,
    step_key,
    step_value,
    step_gate,
):
    sequences, span_rows = (block_input.shape[0], block_input.shape[1])
    local_width = key_weight.shape[1]
    local_heads = local_width // HEAD_DIM
    shares = sequences * GROUP
    past_parts = past_gates.reshape(sequences, local_heads, GROUP, -1)
    block_parts = block_gates.reshape(sequences, local_heads, GROUP, -1)
    gate_block_groups = (
        jnp.concatenate([past_parts, block_parts], axis=3)
        .transpose(0, 2, 1, 3)
        .reshape(shares, local_heads, -1)
    )
    cache_gates = lax.all_to_all(gate_block_groups, "sp", split_axis=0, concat_axis=2, tiled=True)
    gathered = lax.all_gather(block_input, "tp", axis=2, tiled=True)
    flat_input = gathered.reshape(sequences * span_rows, gathered.shape[2])
    key_sums = jnp.dot(
        flat_input,
        lax.all_gather(key_weight, "sp", axis=0, tiled=True),
        preferred_element_type=jnp.float32,
    )
    value_sums = jnp.dot(
        flat_input,
        lax.all_gather(value_weight, "sp", axis=0, tiled=True),
        preferred_element_type=jnp.float32,
    )
    block_keys = key_sums.astype(jnp.bfloat16).reshape(sequences, span_rows, local_width)
    block_values = value_sums.astype(jnp.bfloat16).reshape(sequences, span_rows, local_width)
    joined_keys = jnp.concatenate(
        [share_split(earlier_keys, shares), share_split(block_keys, shares)], axis=1
    )
    assembled_vector_entries = jnp.concatenate(
        [share_split(past_values, shares), share_split(block_values, shares)], axis=1
    )
    cache_keys, stored_vector_entries = (
        lax.all_to_all(joined_keys, "sp", split_axis=0, concat_axis=1, tiled=True),
        lax.all_to_all(assembled_vector_entries, "sp", split_axis=0, concat_axis=1, tiled=True),
    )
    queries = step_query.reshape(sequences, local_heads, HEAD_DIM)
    owner_seq = lax.axis_index("sp") // GROUP
    own_query = lax.dynamic_slice_in_dim(queries, owner_seq, 1, 0)
    own_gate = lax.dynamic_slice_in_dim(step_gate, owner_seq, 1, 0)
    maximum, denominator, summed = partial_read(
        own_query, cache_keys, stored_vector_entries, cache_gates, own_gate
    )
    chosen = (jnp.arange(sequences, dtype=jnp.int32) == owner_seq)[:, None]
    partial_value = (
        jnp.where(chosen, maximum, lowest_score_bound),
        jnp.where(chosen, denominator, 0.0),
        jnp.where(chosen[:, :, None], summed, 0.0),
    )
    merged = merged_2(partial_value, "sp", combine_reads)
    own_keys = step_key.reshape(sequences, local_heads, HEAD_DIM).astype(jnp.float32)
    own_values = step_value.reshape(sequences, local_heads, HEAD_DIM).astype(jnp.float32)
    own_score = jnp.sum(queries.astype(jnp.float32) * own_keys, axis=2) * HEAD_DIM ** (-0.5)
    maximum = jnp.maximum(merged[0], own_score)
    kept_scale = jnp.exp(merged[0] - maximum)
    fresh_weight = jnp.exp(own_score - maximum)
    denominator = merged[1] * kept_scale + fresh_weight
    summed = merged[2] * kept_scale[:, :, None] + fresh_weight[:, :, None] * own_values
    initial_attention_output = (summed / denominator[:, :, None]).reshape(sequences, local_width)
    return (cache_keys, stored_vector_entries, cache_gates, initial_attention_output)


MESH = pl.DeviceIdType.MESH
F32 = jnp.float32
BF16 = jnp.bfloat16
CHUNKS = 4


def nt_dot(a, b):
    return lax.dot_general(a, b, (((1,), (1,)), ((), ())), preferred_element_type=F32)


def iotas(rows, columns):
    return (
        lax.broadcasted_iota(jnp.int32, (rows, columns), 0),
        lax.broadcasted_iota(jnp.int32, (rows, columns), 1),
    )


def permuted(rows, row_source):
    count = rows.shape[0]
    target, source = iotas(count, count)
    one_hot = jnp.where(source == row_source(target), 1.0, 0.0).astype(BF16)
    return jnp.dot(one_hot, rows, preferred_element_type=F32).astype(BF16)


def diagonal_blocks(full, heads):
    width = full.shape[1] // heads
    row, _ = iotas(heads, width)
    total = jnp.zeros((heads, width), F32)
    for head in range(heads):
        total = jnp.where(row == head, full[:, head * width : (head + 1) * width], total)
    return total


def block_read(query_diagonal, keys, values, gates, gate_here, heads):
    head_width = keys.shape[1] // heads
    scores = nt_dot(query_diagonal, keys) * head_width ** (-0.5) + gate_here - gates
    maximum = jnp.max(scores, axis=1, keepdims=True)
    weights = jnp.exp(scores - maximum)
    denominator = jnp.sum(weights, axis=1, keepdims=True)
    upper = weights.astype(BF16)
    lower = (weights - upper.astype(F32)).astype(BF16)
    full = jnp.dot(upper, values, preferred_element_type=F32) + jnp.dot(
        lower, values, preferred_element_type=F32
    )
    return maximum, denominator, diagonal_blocks(full, heads)


def merge_pair(one, two):
    maximum = jnp.maximum(one[0], two[0])
    scale_one = jnp.exp(one[0] - maximum)
    scale_two = jnp.exp(two[0] - maximum)
    return (
        maximum,
        one[1] * scale_one + two[1] * scale_two,
        one[2] * scale_one + two[2] * scale_two,
    )


def kernel(
    n, tp, plane, dims,
    x_ref, wk_ref, wv_ref, ek_ref, pv_ref, gg_ref, pg_ref, q_ref, sk_ref, sv_ref, sg_ref,
    ck_ref, cv_ref, cg_ref, out_ref,
    xp, xr, w, pf, ps, pr, pk, pv, gr, st, sr, kb, vb,
    x_send, x_recv, w_send, w_recv, p_send, p_recv, r_send, r_recv, s_send, s_recv,
):
    span, past_rows, block_rows, width, heads = dims
    depth = n // plane
    me = lax.axis_index("sp")
    core = lax.axis_index("tp")
    z, p = me // plane, me % plane
    shares = n
    per = past_rows + block_rows
    chunk = 2 * width // CHUNKS
    per_matrix = width // chunk
    features = xr.shape[2]

    barrier = pltpu.get_barrier_semaphore()
    for k in range(n):
        for j in range(tp):
            if k or j:
                pl.semaphore_signal(
                    barrier, inc=1,
                    device_id=((me + k) % n, (core + j) % tp), device_id_type=MESH,
                )
    xp[...] = permuted(
        x_ref[...],
        lambda r: ((r % (depth * block_rows)) // block_rows * plane + r // (depth * block_rows)) * block_rows
        + r % block_rows,
    )
    for c in range(CHUNKS):
        weight = wk_ref if c < per_matrix else wv_ref
        base = (c % per_matrix) * chunk
        w[c, p] = weight[:, base : base + chunk]
    pk[me] = ek_ref[me]
    pv[me] = pv_ref[me]
    gr[me] = gg_ref[me]
    pl.semaphore_wait(barrier, n * tp - 1)

    rows_each = depth * block_rows
    z_each = depth // tp
    pending = []
    for zz in range(z_each):
        for q in range(plane):
            target = (core * z_each + zz) * plane + q
            source = xp.at[q * rows_each : (q + 1) * rows_each, zz * features : (zz + 1) * features]
            for j in range(tp):
                index = (zz * plane + q) * tp + j
                copy = pltpu.make_async_remote_copy(
                    src_ref=source, dst_ref=xr.at[me],
                    send_sem=x_send.at[index], recv_sem=x_recv.at[me],
                    device_id=(target, (core + j) % tp), device_id_type=MESH,
                )
                if j:
                    copy.start()
                    pending.append(copy)
                else:
                    own = pltpu.make_async_copy(source, xr.at[me], x_recv.at[me])

                    @pl.when(target != me)
                    def _(copy=copy):
                        copy.start()

                    @pl.when(target == me)
                    def _(own=own):
                        own.start()

    def send_weights(c):
        weight = wk_ref if c < per_matrix else wv_ref
        base = (c % per_matrix) * chunk
        copies = []
        for k in range(1, plane):
            copy = pltpu.make_async_remote_copy(
                src_ref=weight.at[:, base : base + chunk], dst_ref=w.at[c, p],
                send_sem=w_send.at[c, k], recv_sem=w_recv.at[c, k],
                device_id=(z * plane + (p + k) % plane, core), device_id_type=MESH,
            )
            copy.start()
            copies.append(copy)
        return copies

    def send_past(which, source_ref, target_ref):
        copies = []
        for k in range(1, n):
            target = (me + k) % n
            copy = pltpu.make_async_remote_copy(
                src_ref=source_ref.at[target], dst_ref=target_ref.at[me],
                send_sem=p_send.at[which, k], recv_sem=p_recv.at[which, k],
                device_id=(target, core), device_id_type=MESH,
            )
            copy.start()
            copies.append(copy)
        return copies

    weight_copies = [send_weights(0)]
    gate_copies = send_past(2, gg_ref, gr)
    key_copies = send_past(0, ek_ref, pk)
    weight_copies.append(send_weights(1))
    value_copies = send_past(1, pv_ref, pv)
    for c in range(2, CHUNKS):
        weight_copies.append(send_weights(c))

    row, column = iotas(heads, width)
    query = q_ref[...].astype(F32)
    query_diagonal = jnp.where(
        column // (width // heads) == row, jnp.concatenate([query] * heads, axis=1), 0.0
    ).astype(BF16)
    gate_here = sg_ref[:, 0:1]
    read = block_read(
        query_diagonal,
        ek_ref[...].reshape(n * past_rows, width),
        pv_ref[...].reshape(n * past_rows, width),
        pg_ref[...], gate_here, heads,
    )

    for i in range(n):
        pltpu.make_async_copy(xr.at[i], xr.at[i], x_recv.at[i]).wait()
    inputs = permuted(
        xr[...].reshape(n * rows_each, features),
        lambda r: (r % (n * block_rows)) // block_rows * rows_each
        + r // (n * block_rows) * block_rows + r % block_rows,
    )
    group_rows = n * block_rows
    partial_copies = []

    def finish(c):
        total = pf[c % 2, pl.ds(pl.multiple_of(z * group_rows, group_rows), group_rows), :]
        for k in range(1, depth):
            partial_copies[c][k - 1].wait_recv()
            total = total + pr[c, k].astype(F32)
        base = (c % per_matrix) * chunk
        block = kb if c < per_matrix else vb
        block[:, base : base + chunk] = total.astype(BF16)

    for c in range(CHUNKS):
        for copy in weight_copies[c]:
            copy.wait_recv()
        product = jnp.dot(inputs, w[c].reshape(plane * w.shape[2], chunk), preferred_element_type=F32)
        pf[c % 2] = product
        ps[c] = product.astype(BF16).reshape(depth, group_rows, chunk)
        copies = []
        for k in range(1, depth):
            target = (z + k) % depth
            copy = pltpu.make_async_remote_copy(
                src_ref=ps.at[c, target], dst_ref=pr.at[c, k],
                send_sem=r_send.at[c, k], recv_sem=r_recv.at[c, k],
                device_id=(target * plane + p, core), device_id_type=MESH,
            )
            copy.start()
            copies.append(copy)
        partial_copies.append(copies)
        if c:
            finish(c - 1)
    for copy in gate_copies:
        copy.wait_recv()
    _, lane = iotas(heads, gr.shape[2])
    gates = jnp.zeros((heads, gr.shape[2]), F32)
    for i in range(n):
        shift = (i * block_rows - past_rows) % gr.shape[2]
        moved = pltpu.roll(gr[i], shift, 1) if shift else gr[i]
        gates = jnp.where(lane // block_rows == i, moved, gates)
    finish(CHUNKS - 1)

    read = merge_pair(
        read,
        block_read(query_diagonal, kb[...], vb[...], gates[:, :group_rows], gate_here, heads),
    )
    half = st.shape[1] // 2
    _, lane = iotas(heads, st.shape[1])
    st[0:heads, :] = jnp.where(lane < half, read[0], read[1])
    st[heads : 2 * heads, :] = read[2]
    stat_copies = []
    for k in range(1, n):
        copy = pltpu.make_async_remote_copy(
            src_ref=st, dst_ref=sr.at[k],
            send_sem=s_send.at[k], recv_sem=s_recv.at[k],
            device_id=((me + k) % n, core), device_id_type=MESH,
        )
        copy.start()
        stat_copies.append(copy)

    def assembled(past, block):
        rows = jnp.concatenate([past.reshape(n * past_rows, width), block], axis=0)

        def row_source(r):
            source, place = r // per, r % per
            return jnp.where(
                place < past_rows,
                source * past_rows + place,
                n * past_rows + source * block_rows + place - past_rows,
            )

        return permuted(rows, row_source)

    for copy in key_copies:
        copy.wait_recv()
    ck_ref[...] = assembled(pk[...], kb[...])
    for copy in value_copies:
        copy.wait_recv()
    cv_ref[...] = assembled(pv[...], vb[...])
    cg_ref[...] = gr[...]

    own_score = jnp.sum(query * sk_ref[...].astype(F32), axis=1, keepdims=True) * (
        (width // heads) ** (-0.5)
    )
    read = merge_pair(read, (own_score, jnp.ones_like(own_score), sv_ref[...].astype(F32)))
    for copy in stat_copies:
        copy.wait_recv()
    for k in range(1, n):
        read = merge_pair(
            read, (sr[k, 0:heads, 0:1], sr[k, 0:heads, half : half + 1], sr[k, heads : 2 * heads, :])
        )
    out_ref[...] = read[2] / read[1]

    for zz in range(z_each):
        for q in range(plane):
            target = (core * z_each + zz) * plane + q
            index = (zz * plane + q) * tp
            source = xp.at[q * rows_each : (q + 1) * rows_each, zz * features : (zz + 1) * features]

            @pl.when(target != me)
            def _(source=source, index=index):
                pltpu.make_async_copy(source, source, x_send.at[index]).wait()

    for copy in pending:
        copy.wait_send()
    for copies in weight_copies + partial_copies + [gate_copies, key_copies, value_copies, stat_copies]:
        for copy in copies:
            copy.wait_send()


def fused(
    n, tp, plane,
    block_input, key_weight, value_weight, earlier_keys, past_values, past_gates, block_gates,
    step_query, step_key, step_value, step_gate,
):
    span, features_here = block_input.shape[1:]
    kept, width = key_weight.shape
    heads = width // HEAD_DIM
    past_rows = earlier_keys.shape[1] // n
    block_rows = span // n
    depth = n // plane
    per = past_rows + block_rows
    lanes = HEAD_DIM
    grouped = jnp.concatenate(
        [
            past_gates.reshape(heads, n, past_rows),
            block_gates.reshape(heads, n, block_rows),
            jnp.zeros((heads, n, lanes - per), F32),
        ],
        axis=2,
    ).transpose(1, 0, 2)
    chunk = 2 * width // CHUNKS
    group_rows = n * block_rows
    dims = (span, past_rows, block_rows, width, heads)
    vmem = pl.BlockSpec(memory_space=pltpu.VMEM)
    dma = pltpu.SemaphoreType.DMA
    keys, values, gates, read = pl.pallas_call(
        functools.partial(kernel, n, tp, plane, dims),
        name="relay",
        out_shape=(
            jax.ShapeDtypeStruct((n * per, width), BF16),
            jax.ShapeDtypeStruct((n * per, width), BF16),
            jax.ShapeDtypeStruct((n, heads, lanes), F32),
            jax.ShapeDtypeStruct((heads, HEAD_DIM), F32),
        ),
        in_specs=[vmem] * 11,
        out_specs=(vmem,) * 4,
        scratch_shapes=[
            pltpu.VMEM((span, features_here), BF16),
            pltpu.VMEM((n, depth * block_rows, plane * kept), BF16),
            pltpu.VMEM((CHUNKS, plane, kept, chunk), BF16),
            pltpu.VMEM((2, depth * group_rows, chunk), F32),
            pltpu.VMEM((CHUNKS, depth, group_rows, chunk), BF16),
            pltpu.VMEM((CHUNKS, depth, group_rows, chunk), BF16),
            pltpu.VMEM((n, past_rows, width), BF16),
            pltpu.VMEM((n, past_rows, width), BF16),
            pltpu.VMEM((n, heads, lanes), F32),
            pltpu.VMEM((2 * heads, HEAD_DIM), F32),
            pltpu.VMEM((n, 2 * heads, HEAD_DIM), F32),
            pltpu.VMEM((group_rows, width), BF16),
            pltpu.VMEM((group_rows, width), BF16),
            dma((depth // tp * plane * tp,)),
            dma((n,)),
            dma((CHUNKS, plane)),
            dma((CHUNKS, plane)),
            dma((3, n)),
            dma((3, n)),
            dma((CHUNKS, depth)),
            dma((CHUNKS, depth)),
            dma((n,)),
            dma((n,)),
        ],
        compiler_params=pltpu.CompilerParams(
            collective_id=0, has_side_effects=True, vmem_limit_bytes=48 * 1024 * 1024
        ),
    )(
        block_input[0],
        key_weight,
        value_weight,
        earlier_keys.reshape(n, past_rows, width),
        past_values.reshape(n, past_rows, width),
        grouped,
        past_gates[0],
        step_query.reshape(heads, HEAD_DIM),
        step_key.reshape(heads, HEAD_DIM),
        step_value.reshape(heads, HEAD_DIM),
        jnp.broadcast_to(step_gate.reshape(heads, 1), (heads, lanes)),
    )
    cache_gates = gates[:, :, :per].transpose(1, 0, 2).reshape(1, heads, n * per)
    return keys[None], values[None], cache_gates, read.reshape(1, width)


def plane_size(n):
    plane = 1
    while 4 * plane * plane <= n:
        plane *= 2
    return plane


def fits(n, tp, args):
    block_input, key_weight, earlier_keys = args[0], args[1], args[3]
    plane = plane_size(n)
    depth = n // plane
    span, width = block_input.shape[1], key_weight.shape[1]
    heads = width // HEAD_DIM
    past_rows, block_rows = earlier_keys.shape[1] // n, span // n
    return (
        block_input.shape[0] == 1 and n == GROUP and n % plane == 0 and depth % tp == 0
        and span % n == 0 and past_rows % 16 == 0 and (depth * block_rows) % 16 == 0
        and past_rows + block_rows <= HEAD_DIM and n * block_rows <= HEAD_DIM
        and heads % 8 == 0 and width % (CHUNKS // 2 * HEAD_DIM) == 0
    )


def local_program(n, tp, *args):
    if fits(n, tp, args):
        return fused(n, tp, plane_size(n), *args)
    return local(*args)


def solution(mesh):
    in_specs = (
        P(None, "sp", "tp"),
        P("sp", "tp"),
        P("sp", "tp"),
        P(None, "sp", "tp"),
        P(None, "sp", "tp"),
        P(None, "tp", "sp"),
        P(None, "tp", "sp"),
        P(None, "tp"),
        P(None, "tp"),
        P(None, "tp"),
        P(None, "tp"),
    )
    out_specs = (P("sp", None, "tp"), P("sp", None, "tp"), P("sp", "tp", None), P(None, "tp"))
    body = functools.partial(local_program, mesh.shape["sp"], mesh.shape["tp"])
    return jax.shard_map(body, mesh=mesh, in_specs=in_specs, out_specs=out_specs, check_vma=False)
```

```python
import functools

import jax
import jax.numpy as jnp
from jax import lax
from jax.experimental import pallas as pl
from jax.experimental.pallas import tpu as pltpu
from jax.sharding import PartitionSpec as P

HEAD_DIM = 128
GROUP = 16


lowest_score_bound = -1e30


def merged_2(part, axis, combine):
    gathered = jax.tree.map(lambda a: lax.all_gather(a, axis), part)

    def take(source):
        return jax.tree.map(lambda a: lax.dynamic_index_in_dim(a, source, 0, False), gathered)

    return lax.fori_loop(
        1, lax.axis_size(axis), lambda source, state: combine(state, take(source)), take(0)
    )


def share_split(source_rows, shares):
    return source_rows.reshape(shares, -1, source_rows.shape[2])


def partial_read(queries, key_rows, value_rows, gate_rows, gate_here):
    sequences, row_count = (key_rows.shape[0], key_rows.shape[1])
    local_heads, head_width = (queries.shape[1], queries.shape[2])
    key_rows = key_rows.reshape(sequences, row_count, local_heads, head_width)
    value_rows = value_rows.reshape(sequences, row_count, local_heads, head_width)
    scores = jnp.einsum("shd,srhd->shr", queries, key_rows, preferred_element_type=jnp.float32)
    scores = scores * head_width ** (-0.5) + gate_here[:, :, None] - gate_rows
    maximum = jnp.max(scores, axis=2)
    weights = jnp.exp(scores - maximum[:, :, None])
    denominator = jnp.sum(weights, axis=2)
    summed = jnp.einsum(
        "shr,srhd->shd", weights, value_rows.astype(jnp.float32), precision=lax.Precision.HIGHEST
    )
    return (maximum, denominator, summed)


def combine_reads(former, latter):
    maximum = jnp.maximum(former[0], latter[0])
    former_scale = jnp.exp(former[0] - maximum)
    latter_scale = jnp.exp(latter[0] - maximum)
    return (
        maximum,
        former[1] * former_scale + latter[1] * latter_scale,
        former[2] * former_scale[:, :, None] + latter[2] * latter_scale[:, :, None],
    )


def local(
    block_input,
    key_weight,
    value_weight,
    earlier_keys,
    past_values,
    past_gates,
    block_gates,
    step_query,
    step_key,
    step_value,
    step_gate,
):
    sequences, span_rows = (block_input.shape[0], block_input.shape[1])
    local_width = key_weight.shape[1]
    local_heads = local_width // HEAD_DIM
    shares = sequences * GROUP
    past_parts = past_gates.reshape(sequences, local_heads, GROUP, -1)
    block_parts = block_gates.reshape(sequences, local_heads, GROUP, -1)
    gate_block_groups = (
        jnp.concatenate([past_parts, block_parts], axis=3)
        .transpose(0, 2, 1, 3)
        .reshape(shares, local_heads, -1)
    )
    cache_gates = lax.all_to_all(gate_block_groups, "sp", split_axis=0, concat_axis=2, tiled=True)
    gathered = lax.all_gather(block_input, "tp", axis=2, tiled=True)
    flat_input = gathered.reshape(sequences * span_rows, gathered.shape[2])
    key_sums = jnp.dot(
        flat_input,
        lax.all_gather(key_weight, "sp", axis=0, tiled=True),
        preferred_element_type=jnp.float32,
    )
    value_sums = jnp.dot(
        flat_input,
        lax.all_gather(value_weight, "sp", axis=0, tiled=True),
        preferred_element_type=jnp.float32,
    )
    block_keys = key_sums.astype(jnp.bfloat16).reshape(sequences, span_rows, local_width)
    block_values = value_sums.astype(jnp.bfloat16).reshape(sequences, span_rows, local_width)
    joined_keys = jnp.concatenate(
        [share_split(earlier_keys, shares), share_split(block_keys, shares)], axis=1
    )
    assembled_vector_entries = jnp.concatenate(
        [share_split(past_values, shares), share_split(block_values, shares)], axis=1
    )
    cache_keys, stored_vector_entries = (
        lax.all_to_all(joined_keys, "sp", split_axis=0, concat_axis=1, tiled=True),
        lax.all_to_all(assembled_vector_entries, "sp", split_axis=0, concat_axis=1, tiled=True),
    )
    queries = step_query.reshape(sequences, local_heads, HEAD_DIM)
    owner_seq = lax.axis_index("sp") // GROUP
    own_query = lax.dynamic_slice_in_dim(queries, owner_seq, 1, 0)
    own_gate = lax.dynamic_slice_in_dim(step_gate, owner_seq, 1, 0)
    maximum, denominator, summed = partial_read(
        own_query, cache_keys, stored_vector_entries, cache_gates, own_gate
    )
    chosen = (jnp.arange(sequences, dtype=jnp.int32) == owner_seq)[:, None]
    partial_value = (
        jnp.where(chosen, maximum, lowest_score_bound),
        jnp.where(chosen, denominator, 0.0),
        jnp.where(chosen[:, :, None], summed, 0.0),
    )
    merged = merged_2(partial_value, "sp", combine_reads)
    own_keys = step_key.reshape(sequences, local_heads, HEAD_DIM).astype(jnp.float32)
    own_values = step_value.reshape(sequences, local_heads, HEAD_DIM).astype(jnp.float32)
    own_score = jnp.sum(queries.astype(jnp.float32) * own_keys, axis=2) * HEAD_DIM ** (-0.5)
    maximum = jnp.maximum(merged[0], own_score)
    kept_scale = jnp.exp(merged[0] - maximum)
    fresh_weight = jnp.exp(own_score - maximum)
    denominator = merged[1] * kept_scale + fresh_weight
    summed = merged[2] * kept_scale[:, :, None] + fresh_weight[:, :, None] * own_values
    initial_attention_output = (summed / denominator[:, :, None]).reshape(sequences, local_width)
    return (cache_keys, stored_vector_entries, cache_gates, initial_attention_output)


MESH = pl.DeviceIdType.MESH
F32 = jnp.float32
BF16 = jnp.bfloat16
CHUNKS = 4


def nt_dot(a, b):
    return lax.dot_general(a, b, (((1,), (1,)), ((), ())), preferred_element_type=F32)


def iotas(rows, columns):
    return (
        lax.broadcasted_iota(jnp.int32, (rows, columns), 0),
        lax.broadcasted_iota(jnp.int32, (rows, columns), 1),
    )


def permuted(rows, row_source):
    count = rows.shape[0]
    target, source = iotas(count, count)
    one_hot = jnp.where(source == row_source(target), 1.0, 0.0).astype(BF16)
    return jnp.dot(one_hot, rows, preferred_element_type=F32).astype(BF16)


def diagonal_blocks(full, heads):
    width = full.shape[1] // heads
    row, _ = iotas(heads, width)
    total = jnp.zeros((heads, width), F32)
    for head in range(heads):
        total = jnp.where(row == head, full[:, head * width : (head + 1) * width], total)
    return total


def block_read(query_diagonal, keys, values, gates, gate_here, heads):
    head_width = keys.shape[1] // heads
    scores = nt_dot(query_diagonal, keys) * head_width ** (-0.5) + gate_here - gates
    maximum = jnp.max(scores, axis=1, keepdims=True)
    weights = jnp.exp(scores - maximum)
    denominator = jnp.sum(weights, axis=1, keepdims=True)
    upper = weights.astype(BF16)
    lower = (weights - upper.astype(F32)).astype(BF16)
    full = jnp.dot(upper, values, preferred_element_type=F32) + jnp.dot(
        lower, values, preferred_element_type=F32
    )
    return maximum, denominator, diagonal_blocks(full, heads)


def merge_pair(one, two):
    maximum = jnp.maximum(one[0], two[0])
    scale_one = jnp.exp(one[0] - maximum)
    scale_two = jnp.exp(two[0] - maximum)
    return (
        maximum,
        one[1] * scale_one + two[1] * scale_two,
        one[2] * scale_one + two[2] * scale_two,
    )


def kernel(
    n, tp, plane, dims,
    x_hbm, wk_hbm, wv_hbm, ek_hbm, pv_hbm, pg_ref, bg_ref, q_ref, sk_ref, sv_ref, sg_ref,
    ck_ref, cv_ref, cg_ref, out_ref,
    x_ref, ek_ref, pv_ref, gg_ref, xp, xr, w, pf, ps, pa, sb, pb, pk, pv, gr, st, sr, kb, vb,
    l_sem, x_send, x_recv, f_send, f_recv, w_send, w_recv, p_send, p_recv, r_send, r_recv, s_send, s_recv,
):
    span, past_rows, block_rows, width, heads = dims
    head_width = width // heads
    depth = n // plane
    pairs = depth // 2
    me = lax.axis_index("sp")
    core = lax.axis_index("tp")
    z, p = me // plane, me % plane
    across, along, corner = p // 2 * 2 + 1 - p % 2, (p + 2) % plane, (p // 2 * 2 + 3 - p % 2) % plane
    per = past_rows + block_rows
    chunk = 2 * width // CHUNKS
    per_matrix = width // chunk
    features = xr.shape[2]
    half_rows = w.shape[2] // 2
    lanes = gg_ref.shape[2]

    loads = [
        pltpu.make_async_copy(x_hbm, x_ref, l_sem.at[0]),
        pltpu.make_async_copy(ek_hbm, ek_ref, l_sem.at[1]),
        pltpu.make_async_copy(pv_hbm, pv_ref, l_sem.at[2]),
    ]
    for c in range(CHUNKS):
        weight = wk_hbm if c < per_matrix else wv_hbm
        base = (c % per_matrix) * chunk
        loads.append(
            pltpu.make_async_copy(weight.at[:, base : base + chunk], w.at[c, p], l_sem.at[3 + c])
        )
    for load in loads:
        load.start()
    barrier = pltpu.get_barrier_semaphore()
    for k in range(n):
        for j in range(tp):
            if k or j:
                pl.semaphore_signal(
                    barrier, inc=1,
                    device_id=((me + k) % n, (core + j) % tp), device_id_type=MESH,
                )
    _, lane = iotas(heads, lanes)
    block_gates = bg_ref[...]
    block_gates = jnp.concatenate([block_gates] * (lanes // block_gates.shape[1]), axis=1)
    for g in range(n):
        start = g * past_rows
        early = pg_ref[:, start // lanes * lanes : start // lanes * lanes + lanes]
        early = pltpu.roll(early, -start % lanes, 1) if start % lanes else early
        shift = (past_rows - g * block_rows) % lanes
        late = pltpu.roll(block_gates, shift, 1) if shift else block_gates
        gg_ref[g] = jnp.where(lane < past_rows, early, late)
    loads[0].wait()
    xp[...] = permuted(
        x_ref[...],
        lambda r: ((r % (depth * block_rows)) // block_rows * plane + r // (depth * block_rows)) * block_rows
        + r % block_rows,
    )
    for load in loads[1:]:
        load.wait()
    pk[me] = ek_ref[me]
    pv[me] = pv_ref[me]
    gr[me] = gg_ref[me]
    pl.semaphore_wait(barrier, n * tp - 1)

    rows_each = depth * block_rows
    z_each = depth // tp

    def input_copy(zz, q):
        target = (core * z_each + zz) * plane + q
        source = xp.at[q * rows_each : (q + 1) * rows_each, zz * features : (zz + 1) * features]
        index = zz * plane + q
        remote = pltpu.make_async_remote_copy(
            src_ref=source, dst_ref=xr.at[me],
            send_sem=x_send.at[index], recv_sem=x_recv.at[me],
            device_id=(target, core), device_id_type=MESH,
        )
        return target, remote, pltpu.make_async_copy(source, xr.at[me], x_recv.at[me])

    for zz in range(z_each):
        for q in range(plane):
            target, remote, own = input_copy(zz, q)

            @pl.when(target != me)
            def _(remote=remote):
                remote.start()

            @pl.when(target == me)
            def _(own=own):
                own.start()

    def remote_weight(c, slot, source, to):
        copy = pltpu.make_async_remote_copy(
            src_ref=source, dst_ref=source,
            send_sem=w_send.at[c, slot], recv_sem=w_recv.at[c, slot],
            device_id=(z * plane + to, core), device_id_type=MESH,
        )
        copy.start()
        return copy

    def send_weights(c):
        return [
            remote_weight(c, 0, w.at[c, p], across),
            remote_weight(c, 1, w.at[c, p], along),
        ]

    def forward_weights(c):
        first, second = w.at[c, across, 0:half_rows], w.at[c, along, half_rows : 2 * half_rows]
        weight_copies[c][0].wait_recv()
        one = remote_weight(c, 2, first, along)
        weight_copies[c][1].wait_recv()
        return [one, remote_weight(c, 3, second, across)]

    def await_corner(c):
        for slot, low in ((2, 0), (3, half_rows)):
            place = w.at[c, corner, low : low + half_rows]
            pltpu.make_async_copy(place, place, w_recv.at[c, slot]).wait()

    def send_past(which, source_ref, target_ref, offsets):
        copies = []
        for k in offsets:
            target = (me + k) % n
            copy = pltpu.make_async_remote_copy(
                src_ref=source_ref.at[target], dst_ref=target_ref.at[me],
                send_sem=p_send.at[which, k], recv_sem=p_recv.at[which, k],
                device_id=(target, core), device_id_type=MESH,
            )
            copy.start()
            copies.append(copy)
        return copies

    others = list(range(1, n))
    key_copies = send_past(0, ek_ref, pk, others)
    weight_copies = [send_weights(0)]
    gate_copies = send_past(2, gg_ref, gr, others)
    weight_copies.append(send_weights(1))

    row, column = iotas(heads, width)
    query_wide = jnp.broadcast_to(q_ref[...].astype(F32), (heads, width))
    query_diagonal = jnp.where(column // head_width == row, query_wide, 0.0).astype(BF16)
    query = diagonal_blocks(query_wide, heads)
    own_key = diagonal_blocks(jnp.broadcast_to(sk_ref[...].astype(F32), (heads, width)), heads)
    own_value = diagonal_blocks(jnp.broadcast_to(sv_ref[...].astype(F32), (heads, width)), heads)
    head_row, head_column = iotas(heads, heads)
    gate_here = jnp.sum(
        jnp.where(head_row == head_column, jnp.broadcast_to(sg_ref[...], (heads, heads)), 0.0),
        axis=1, keepdims=True,
    )
    read = block_read(
        query_diagonal,
        ek_ref[...].reshape(n * past_rows, width),
        pv_ref[...].reshape(n * past_rows, width),
        pg_ref[...], gate_here, heads,
    )

    holder = z // z_each
    handed = [
        pltpu.make_async_remote_copy(
            src_ref=xr, dst_ref=xr, send_sem=f_send.at[j], recv_sem=f_recv.at[j],
            device_id=(me, (core + j) % tp), device_id_type=MESH,
        )
        for j in range(1, tp)
    ]

    @pl.when(core == holder)
    def _():
        for i in range(n):
            pltpu.make_async_copy(xr.at[i], xr.at[i], x_recv.at[i]).wait()
        for copy in handed:
            copy.start()

    for j in range(1, tp):

        @pl.when((holder + j) % tp == core)
        def _(j=j):
            handed[j - 1].wait_recv()

    inputs = permuted(
        xr[...].reshape(n * rows_each, features),
        lambda r: (r % (n * block_rows)) // block_rows * rows_each
        + r // (n * block_rows) * block_rows + r % block_rows,
    )
    group_rows = n * block_rows
    forwards, first_copies, second_copies = [], [], []
    pair, bit = z // 2, z % 2
    mate = pair * 2 + 1 - bit

    def partial_copy(c, slot, source, target_ref, to):
        copy = pltpu.make_async_remote_copy(
            src_ref=source, dst_ref=target_ref,
            send_sem=r_send.at[c, slot], recv_sem=r_recv.at[c, slot],
            device_id=(to * plane + p, core), device_id_type=MESH,
        )
        copy.start()
        return copy

    def own_rows(c, owner):
        return pf[c, pl.ds(pl.multiple_of(owner * group_rows, group_rows), group_rows), :]

    def multiply(c):
        await_corner(c)
        product = jnp.dot(inputs, w[c].reshape(plane * w.shape[2], chunk), preferred_element_type=F32)
        pf[c] = product
        ps[c] = product.astype(BF16).reshape(depth, group_rows, chunk)
        copies = []
        for o in list(range(1, pairs)) + [0]:
            owner = (pair + o) % pairs * 2 + 1 - bit
            copies.append(partial_copy(c, o, ps.at[c, owner], pa.at[c, o], mate))
        first_copies.append(copies)

    def pass_on(c):
        copies = []
        for index, o in enumerate(range(1, pairs)):
            owner = (pair + o) % pairs * 2 + bit
            first_copies[c][index].wait_recv()
            sb[c, o] = (own_rows(c, owner) + pa[c, o].astype(F32)).astype(BF16)
            copies.append(partial_copy(c, pairs + o, sb.at[c, o], pb.at[c, o], owner))
        second_copies.append(copies)

    def finish(c):
        first_copies[c][pairs - 1].wait_recv()
        total = own_rows(c, z) + pa[c, 0].astype(F32)
        for o in range(1, pairs):
            second_copies[c][o - 1].wait_recv()
            total = total + pb[c, o].astype(F32)
        base = (c % per_matrix) * chunk
        block = kb if c < per_matrix else vb
        block[:, base : base + chunk] = total.astype(BF16)

    value_copies = []
    cuts = [len(others) * c // 2 for c in range(3)]
    for c in range(CHUNKS):
        forwards.append(forward_weights(c))
        if c < 2:
            value_copies += send_past(1, pv_ref, pv, others[cuts[c] : cuts[c + 1]])
        if c + 2 < CHUNKS:
            weight_copies.append(send_weights(c + 2))
        if c >= 1:
            multiply(c - 1)
        if c >= 2:
            pass_on(c - 2)
        if c >= 3:
            finish(c - 3)
    multiply(CHUNKS - 1)
    pass_on(CHUNKS - 2)
    finish(CHUNKS - 3)

    for copy in gate_copies:
        copy.wait_recv()
    gates = jnp.zeros((heads, lanes), F32)
    blocks = [jnp.zeros((heads, lanes), F32) for _ in range(pl.cdiv(n * per, lanes))]
    for i in range(n):
        shift = (i * block_rows - past_rows) % lanes
        moved = pltpu.roll(gr[i], shift, 1) if shift else gr[i]
        gates = jnp.where(lane // block_rows == i, moved, gates)
        shift = i * per % lanes
        moved = pltpu.roll(gr[i], shift, 1) if shift else gr[i]
        for number in range(len(blocks)):
            blocks[number] = jnp.where((lane + number * lanes) // per == i, moved, blocks[number])
    for number, values in enumerate(blocks):
        low, high = number * lanes, min((number + 1) * lanes, n * per)
        cg_ref[:, low:high] = values[:, : high - low]

    pass_on(CHUNKS - 1)
    finish(CHUNKS - 2)

    def assembled(past, block):
        rows = jnp.concatenate([past.reshape(n * past_rows, width), block], axis=0)

        def row_source(r):
            source, place = r // per, r % per
            return jnp.where(
                place < past_rows,
                source * past_rows + place,
                n * past_rows + source * block_rows + place - past_rows,
            )

        return permuted(rows, row_source)

    for copy in key_copies:
        copy.wait_recv()
    ck_ref[...] = assembled(pk[...], kb[...])
    own_score = jnp.sum(query * own_key, axis=1, keepdims=True) * head_width ** (-0.5)
    finish(CHUNKS - 1)

    read = merge_pair(
        read,
        block_read(query_diagonal, kb[...], vb[...], gates[:, :group_rows], gate_here, heads),
    )
    half = head_width // 2
    _, lane = iotas(heads, head_width)
    st[0:heads, :] = jnp.where(lane < half, read[0], read[1])
    st[heads : 2 * heads, :] = read[2]
    stat_copies = []
    for k in range(1, n):
        copy = pltpu.make_async_remote_copy(
            src_ref=st, dst_ref=sr.at[k],
            send_sem=s_send.at[k], recv_sem=s_recv.at[k],
            device_id=((me + k) % n, core), device_id_type=MESH,
        )
        copy.start()
        stat_copies.append(copy)

    for copy in value_copies:
        copy.wait_recv()
    cv_ref[...] = assembled(pv[...], vb[...])

    read = merge_pair(read, (own_score, jnp.ones_like(own_score), own_value))
    for copy in stat_copies:
        copy.wait_recv()
    for k in range(1, n):
        read = merge_pair(
            read, (sr[k, 0:heads, 0:1], sr[k, 0:heads, half : half + 1], sr[k, heads : 2 * heads, :])
        )
    result = read[2] / read[1]
    for head in range(heads):
        out_ref[:, head * head_width : (head + 1) * head_width] = result[head : head + 1, :]

    for zz in range(z_each):
        for q in range(plane):
            target, remote, _ = input_copy(zz, q)

            @pl.when(target != me)
            def _(remote=remote):
                remote.wait_send()

    @pl.when(core == holder)
    def _():
        for copy in handed:
            copy.wait_send()

    for copies in (
        weight_copies + forwards + first_copies + second_copies
        + [gate_copies, key_copies, value_copies, stat_copies]
    ):
        for copy in copies:
            copy.wait_send()


def fused(
    n, tp, plane,
    block_input, key_weight, value_weight, earlier_keys, past_values, past_gates, block_gates,
    step_query, step_key, step_value, step_gate,
):
    span, features_here = block_input.shape[1:]
    kept, width = key_weight.shape
    heads = width // HEAD_DIM
    past_rows = earlier_keys.shape[1] // n
    block_rows = span // n
    depth = n // plane
    per = past_rows + block_rows
    lanes = HEAD_DIM
    chunk = 2 * width // CHUNKS
    group_rows = n * block_rows
    dims = (span, past_rows, block_rows, width, heads)
    vmem = pl.BlockSpec(memory_space=pltpu.VMEM)
    hbm = pl.BlockSpec(memory_space=pltpu.HBM)
    dma = pltpu.SemaphoreType.DMA
    rows = pltpu.VMEM((n, past_rows, width), BF16)
    partials = pltpu.VMEM((CHUNKS, depth // 2, group_rows, chunk), BF16)
    keys, values, gates, read = pl.pallas_call(
        functools.partial(kernel, n, tp, plane, dims),
        name="relay",
        out_shape=(
            jax.ShapeDtypeStruct((n * per, width), BF16),
            jax.ShapeDtypeStruct((n * per, width), BF16),
            jax.ShapeDtypeStruct((heads, n * per), F32),
            jax.ShapeDtypeStruct((1, width), F32),
        ),
        in_specs=[hbm] * 5 + [vmem] * 6,
        out_specs=(vmem,) * 4,
        scratch_shapes=[
            pltpu.VMEM((span, features_here), BF16),
            rows,
            rows,
            pltpu.VMEM((n, heads, lanes), F32),
            pltpu.VMEM((span, features_here), BF16),
            pltpu.VMEM((n, depth * block_rows, plane * kept), BF16),
            pltpu.VMEM((CHUNKS, plane, kept, chunk), BF16),
            pltpu.VMEM((CHUNKS, depth * group_rows, chunk), F32),
            pltpu.VMEM((CHUNKS, depth, group_rows, chunk), BF16),
            partials,
            partials,
            partials,
            rows,
            rows,
            pltpu.VMEM((n, heads, lanes), F32),
            pltpu.VMEM((2 * heads, HEAD_DIM), F32),
            pltpu.VMEM((n, 2 * heads, HEAD_DIM), F32),
            pltpu.VMEM((group_rows, width), BF16),
            pltpu.VMEM((group_rows, width), BF16),
            dma((3 + CHUNKS,)),
            dma((depth // tp * plane,)),
            dma((n,)),
            dma((tp,)),
            dma((tp,)),
            dma((CHUNKS, 4)),
            dma((CHUNKS, 4)),
            dma((3, n)),
            dma((3, n)),
            dma((CHUNKS, depth)),
            dma((CHUNKS, depth)),
            dma((n,)),
            dma((n,)),
        ],
        compiler_params=pltpu.CompilerParams(
            collective_id=0, has_side_effects=True, vmem_limit_bytes=48 * 1024 * 1024
        ),
    )(
        block_input[0],
        key_weight,
        value_weight,
        earlier_keys.reshape(n, past_rows, width),
        past_values.reshape(n, past_rows, width),
        past_gates[0],
        block_gates[0],
        step_query,
        step_key,
        step_value,
        step_gate,
    )
    return keys[None], values[None], gates[None], read


def plane_size(n):
    plane = 1
    while 4 * plane * plane <= n:
        plane *= 2
    return plane


def fits(n, tp, args):
    block_input, key_weight, earlier_keys = args[0], args[1], args[3]
    plane = plane_size(n)
    depth = n // plane
    span, width = block_input.shape[1], key_weight.shape[1]
    heads = width // HEAD_DIM
    past_rows, block_rows = earlier_keys.shape[1] // n, span // n
    return (
        block_input.shape[0] == 1 and n == GROUP and plane == 4 and n % plane == 0 and depth % (2 * tp) == 0
        and span % n == 0 and past_rows % 16 == 0 and (depth * block_rows) % 16 == 0
        and HEAD_DIM % past_rows == 0 and past_rows + block_rows <= HEAD_DIM
        and HEAD_DIM % span == 0
        and heads % 8 == 0 and width % (CHUNKS // 2 * HEAD_DIM) == 0
    )


def local_program(n, tp, *args):
    if fits(n, tp, args):
        return fused(n, tp, plane_size(n), *args)
    return local(*args)


def solution(mesh):
    in_specs = (
        P(None, "sp", "tp"),
        P("sp", "tp"),
        P("sp", "tp"),
        P(None, "sp", "tp"),
        P(None, "sp", "tp"),
        P(None, "tp", "sp"),
        P(None, "tp", "sp"),
        P(None, "tp"),
        P(None, "tp"),
        P(None, "tp"),
        P(None, "tp"),
    )
    out_specs = (P("sp", None, "tp"), P("sp", None, "tp"), P("sp", "tp", None), P(None, "tp"))
    body = functools.partial(local_program, mesh.shape["sp"], mesh.shape["tp"])
    return jax.shard_map(body, mesh=mesh, in_specs=in_specs, out_specs=out_specs, check_vma=False)
```

```python
import functools

import jax
import jax.numpy as jnp
from jax import lax
from jax.experimental import pallas as pl
from jax.experimental.pallas import tpu as pltpu
from jax.sharding import PartitionSpec as P

HEAD_DIM = 128
GROUP = 16


lowest_score_bound = -1e30


def merged_2(part, axis, combine):
    gathered = jax.tree.map(lambda a: lax.all_gather(a, axis), part)

    def take(source):
        return jax.tree.map(lambda a: lax.dynamic_index_in_dim(a, source, 0, False), gathered)

    return lax.fori_loop(
        1, lax.axis_size(axis), lambda source, state: combine(state, take(source)), take(0)
    )


def share_split(source_rows, shares):
    return source_rows.reshape(shares, -1, source_rows.shape[2])


def partial_read(queries, key_rows, value_rows, gate_rows, gate_here):
    sequences, row_count = (key_rows.shape[0], key_rows.shape[1])
    local_heads, head_width = (queries.shape[1], queries.shape[2])
    key_rows = key_rows.reshape(sequences, row_count, local_heads, head_width)
    value_rows = value_rows.reshape(sequences, row_count, local_heads, head_width)
    scores = jnp.einsum("shd,srhd->shr", queries, key_rows, preferred_element_type=jnp.float32)
    scores = scores * head_width ** (-0.5) + gate_here[:, :, None] - gate_rows
    maximum = jnp.max(scores, axis=2)
    weights = jnp.exp(scores - maximum[:, :, None])
    denominator = jnp.sum(weights, axis=2)
    summed = jnp.einsum(
        "shr,srhd->shd", weights, value_rows.astype(jnp.float32), precision=lax.Precision.HIGHEST
    )
    return (maximum, denominator, summed)


def combine_reads(former, latter):
    maximum = jnp.maximum(former[0], latter[0])
    former_scale = jnp.exp(former[0] - maximum)
    latter_scale = jnp.exp(latter[0] - maximum)
    return (
        maximum,
        former[1] * former_scale + latter[1] * latter_scale,
        former[2] * former_scale[:, :, None] + latter[2] * latter_scale[:, :, None],
    )


def local(
    block_input,
    key_weight,
    value_weight,
    earlier_keys,
    past_values,
    past_gates,
    block_gates,
    step_query,
    step_key,
    step_value,
    step_gate,
):
    sequences, span_rows = (block_input.shape[0], block_input.shape[1])
    local_width = key_weight.shape[1]
    local_heads = local_width // HEAD_DIM
    shares = sequences * GROUP
    past_parts = past_gates.reshape(sequences, local_heads, GROUP, -1)
    block_parts = block_gates.reshape(sequences, local_heads, GROUP, -1)
    gate_block_groups = (
        jnp.concatenate([past_parts, block_parts], axis=3)
        .transpose(0, 2, 1, 3)
        .reshape(shares, local_heads, -1)
    )
    cache_gates = lax.all_to_all(gate_block_groups, "sp", split_axis=0, concat_axis=2, tiled=True)
    gathered = lax.all_gather(block_input, "tp", axis=2, tiled=True)
    flat_input = gathered.reshape(sequences * span_rows, gathered.shape[2])
    key_sums = jnp.dot(
        flat_input,
        lax.all_gather(key_weight, "sp", axis=0, tiled=True),
        preferred_element_type=jnp.float32,
    )
    value_sums = jnp.dot(
        flat_input,
        lax.all_gather(value_weight, "sp", axis=0, tiled=True),
        preferred_element_type=jnp.float32,
    )
    block_keys = key_sums.astype(jnp.bfloat16).reshape(sequences, span_rows, local_width)
    block_values = value_sums.astype(jnp.bfloat16).reshape(sequences, span_rows, local_width)
    joined_keys = jnp.concatenate(
        [share_split(earlier_keys, shares), share_split(block_keys, shares)], axis=1
    )
    assembled_vector_entries = jnp.concatenate(
        [share_split(past_values, shares), share_split(block_values, shares)], axis=1
    )
    cache_keys, stored_vector_entries = (
        lax.all_to_all(joined_keys, "sp", split_axis=0, concat_axis=1, tiled=True),
        lax.all_to_all(assembled_vector_entries, "sp", split_axis=0, concat_axis=1, tiled=True),
    )
    queries = step_query.reshape(sequences, local_heads, HEAD_DIM)
    owner_seq = lax.axis_index("sp") // GROUP
    own_query = lax.dynamic_slice_in_dim(queries, owner_seq, 1, 0)
    own_gate = lax.dynamic_slice_in_dim(step_gate, owner_seq, 1, 0)
    maximum, denominator, summed = partial_read(
        own_query, cache_keys, stored_vector_entries, cache_gates, own_gate
    )
    chosen = (jnp.arange(sequences, dtype=jnp.int32) == owner_seq)[:, None]
    partial_value = (
        jnp.where(chosen, maximum, lowest_score_bound),
        jnp.where(chosen, denominator, 0.0),
        jnp.where(chosen[:, :, None], summed, 0.0),
    )
    merged = merged_2(partial_value, "sp", combine_reads)
    own_keys = step_key.reshape(sequences, local_heads, HEAD_DIM).astype(jnp.float32)
    own_values = step_value.reshape(sequences, local_heads, HEAD_DIM).astype(jnp.float32)
    own_score = jnp.sum(queries.astype(jnp.float32) * own_keys, axis=2) * HEAD_DIM ** (-0.5)
    maximum = jnp.maximum(merged[0], own_score)
    kept_scale = jnp.exp(merged[0] - maximum)
    fresh_weight = jnp.exp(own_score - maximum)
    denominator = merged[1] * kept_scale + fresh_weight
    summed = merged[2] * kept_scale[:, :, None] + fresh_weight[:, :, None] * own_values
    initial_attention_output = (summed / denominator[:, :, None]).reshape(sequences, local_width)
    return (cache_keys, stored_vector_entries, cache_gates, initial_attention_output)


MESH = pl.DeviceIdType.MESH
F32 = jnp.float32
BF16 = jnp.bfloat16
CHUNKS = 4


def nt_dot(a, b):
    return lax.dot_general(a, b, (((1,), (1,)), ((), ())), preferred_element_type=F32)


def iotas(rows, columns):
    return (
        lax.broadcasted_iota(jnp.int32, (rows, columns), 0),
        lax.broadcasted_iota(jnp.int32, (rows, columns), 1),
    )


def permuted(rows, row_source):
    count = rows.shape[0]
    target, source = iotas(count, count)
    one_hot = jnp.where(source == row_source(target), 1.0, 0.0).astype(BF16)
    return jnp.dot(one_hot, rows, preferred_element_type=F32).astype(BF16)


def diagonal_blocks(full, heads):
    width = full.shape[1] // heads
    row, _ = iotas(heads, width)
    total = jnp.zeros((heads, width), F32)
    for head in range(heads):
        total = jnp.where(row == head, full[:, head * width : (head + 1) * width], total)
    return total


def block_read(query_diagonal, keys, values, gates, gate_here, heads):
    head_width = keys.shape[1] // heads
    scores = nt_dot(query_diagonal, keys) * head_width ** (-0.5) + gate_here - gates
    maximum = jnp.max(scores, axis=1, keepdims=True)
    weights = jnp.exp(scores - maximum)
    denominator = jnp.sum(weights, axis=1, keepdims=True)
    upper = weights.astype(BF16)
    lower = (weights - upper.astype(F32)).astype(BF16)
    full = jnp.dot(upper, values, preferred_element_type=F32) + jnp.dot(
        lower, values, preferred_element_type=F32
    )
    return maximum, denominator, diagonal_blocks(full, heads)


def merge_pair(one, two):
    maximum = jnp.maximum(one[0], two[0])
    scale_one = jnp.exp(one[0] - maximum)
    scale_two = jnp.exp(two[0] - maximum)
    return (
        maximum,
        one[1] * scale_one + two[1] * scale_two,
        one[2] * scale_one + two[2] * scale_two,
    )


def kernel(
    n, tp, plane, dims,
    x_hbm, wk_hbm, wv_hbm, ek_hbm, pv_hbm, pg_ref, bg_ref, q_ref, sk_ref, sv_ref, sg_ref,
    ck_ref, cv_ref, cg_ref, out_ref,
    x_ref, ek_ref, pv_ref, gg_ref, xp, xr, w, pf, ps, pa_k, sb_k, pb_k, pa_v, sb_v, pb_v, tk, tv, pk, pv,
    gr, st, sr, kb, vb,
    l_sem, x_send, x_recv, f_send, f_recv, w_send, w_recv, p_send, p_recv, d_send, d_recv, r_send, r_recv, s_send, s_recv,
):
    span, past_rows, block_rows, width, heads = dims
    head_width = width // heads
    depth = n // plane
    pairs = depth // 2
    me = lax.axis_index("sp")
    core = lax.axis_index("tp")
    z, p = me // plane, me % plane
    across, along, corner = p // 2 * 2 + 1 - p % 2, (p + 2) % plane, (p // 2 * 2 + 3 - p % 2) % plane
    per = past_rows + block_rows
    chunk = 2 * width // CHUNKS
    per_matrix = width // chunk
    features = xr.shape[2]
    half_rows = w.shape[2] // 2
    lanes = gg_ref.shape[2]

    loads = [
        pltpu.make_async_copy(x_hbm, x_ref, l_sem.at[0]),
        pltpu.make_async_copy(ek_hbm, ek_ref, l_sem.at[1]),
        pltpu.make_async_copy(pv_hbm, pv_ref, l_sem.at[2]),
    ]
    for c in range(CHUNKS):
        weight = wk_hbm if c < per_matrix else wv_hbm
        base = (c % per_matrix) * chunk
        loads.append(
            pltpu.make_async_copy(weight.at[:, base : base + chunk], w.at[c, p], l_sem.at[3 + c])
        )
    for load in loads:
        load.start()
    barrier = pltpu.get_barrier_semaphore()
    for k in range(n):
        for j in range(tp):
            if k or j:
                pl.semaphore_signal(
                    barrier, inc=1,
                    device_id=((me + k) % n, (core + j) % tp), device_id_type=MESH,
                )
    _, lane = iotas(heads, lanes)
    block_gates = bg_ref[...]
    block_gates = jnp.concatenate([block_gates] * (lanes // block_gates.shape[1]), axis=1)
    for g in range(n):
        start = g * past_rows
        early = pg_ref[:, start // lanes * lanes : start // lanes * lanes + lanes]
        early = pltpu.roll(early, -start % lanes, 1) if start % lanes else early
        shift = (past_rows - g * block_rows) % lanes
        late = pltpu.roll(block_gates, shift, 1) if shift else block_gates
        gg_ref[g] = jnp.where(lane < past_rows, early, late)
    loads[0].wait()
    xp[...] = permuted(
        x_ref[...],
        lambda r: ((r % (depth * block_rows)) // block_rows * plane + r // (depth * block_rows)) * block_rows
        + r % block_rows,
    )
    for load in loads[1:]:
        load.wait()
    tk[z] = ek_ref[z]
    tv[z] = pv_ref[z]
    gr[me] = gg_ref[me]
    pl.semaphore_wait(barrier, n * tp - 1)

    rows_each = depth * block_rows
    z_each = depth // tp

    def input_copy(zz, q):
        target = (core * z_each + zz) * plane + q
        source = xp.at[q * rows_each : (q + 1) * rows_each, zz * features : (zz + 1) * features]
        index = zz * plane + q
        remote = pltpu.make_async_remote_copy(
            src_ref=source, dst_ref=xr.at[me],
            send_sem=x_send.at[index], recv_sem=x_recv.at[me],
            device_id=(target, core), device_id_type=MESH,
        )
        return target, remote, pltpu.make_async_copy(source, xr.at[me], x_recv.at[me])

    for zz in range(z_each):
        for q in range(plane):
            target, remote, own = input_copy(zz, q)

            @pl.when(target != me)
            def _(remote=remote):
                remote.start()

            @pl.when(target == me)
            def _(own=own):
                own.start()

    def remote_weight(c, slot, source, to):
        copy = pltpu.make_async_remote_copy(
            src_ref=source, dst_ref=source,
            send_sem=w_send.at[c, slot], recv_sem=w_recv.at[c, slot],
            device_id=(z * plane + to, core), device_id_type=MESH,
        )
        copy.start()
        return copy

    def send_weights(c):
        return [
            remote_weight(c, 0, w.at[c, p], across),
            remote_weight(c, 1, w.at[c, p], along),
        ]

    def forward_weights(c):
        first, second = w.at[c, across, 0:half_rows], w.at[c, along, half_rows : 2 * half_rows]
        weight_copies[c][0].wait_recv()
        one = remote_weight(c, 2, first, along)
        weight_copies[c][1].wait_recv()
        return [one, remote_weight(c, 3, second, across)]

    def await_corner(c):
        for slot, low in ((2, 0), (3, half_rows)):
            place = w.at[c, corner, low : low + half_rows]
            pltpu.make_async_copy(place, place, w_recv.at[c, slot]).wait()

    def start_copy(source, target_ref, sends, receives, to):
        copy = pltpu.make_async_remote_copy(
            src_ref=source, dst_ref=target_ref, send_sem=sends, recv_sem=receives,
            device_id=(to, core), device_id_type=MESH,
        )
        copy.start()
        return copy

    def send_bundles(which, source_ref, target_ref):
        return [
            start_copy(
                source_ref.at[(z + k) % depth], target_ref.at[z],
                p_send.at[which, k], p_recv.at[which, k], (z + k) % depth * plane + p,
            )
            for k in range(1, depth)
        ]

    def distribute(which, bundles, source_ref, target_ref):
        for copy in bundles:
            copy.wait_recv()
        copies = [
            start_copy(
                source_ref.at[:, (p + k) % plane], target_ref.at[:, p],
                d_send.at[which, k], d_recv.at[which, k], z * plane + (p + k) % plane,
            )
            for k in range(1, plane)
        ]
        for floor in range(depth):
            target_ref[floor, p] = source_ref[floor, p]
        return copies

    gate_copies = [
        start_copy(
            gg_ref.at[(me + k) % n], gr.at[me],
            d_send.at[2, k], d_recv.at[2, k], (me + k) % n,
        )
        for k in range(1, n)
    ]
    key_bundles = send_bundles(0, ek_ref, tk)
    weight_copies = [send_weights(0), send_weights(1)]
    value_bundles = send_bundles(1, pv_ref, tv)

    row, column = iotas(heads, width)
    query_wide = jnp.broadcast_to(q_ref[...].astype(F32), (heads, width))
    query_diagonal = jnp.where(column // head_width == row, query_wide, 0.0).astype(BF16)
    query = diagonal_blocks(query_wide, heads)
    own_key = diagonal_blocks(jnp.broadcast_to(sk_ref[...].astype(F32), (heads, width)), heads)
    own_value = diagonal_blocks(jnp.broadcast_to(sv_ref[...].astype(F32), (heads, width)), heads)
    head_row, head_column = iotas(heads, heads)
    gate_here = jnp.sum(
        jnp.where(head_row == head_column, jnp.broadcast_to(sg_ref[...], (heads, heads)), 0.0),
        axis=1, keepdims=True,
    )
    read = block_read(
        query_diagonal,
        ek_ref[...].reshape(n * past_rows, width),
        pv_ref[...].reshape(n * past_rows, width),
        pg_ref[...], gate_here, heads,
    )

    holder = z // z_each
    handed = [
        pltpu.make_async_remote_copy(
            src_ref=xr, dst_ref=xr, send_sem=f_send.at[j], recv_sem=f_recv.at[j],
            device_id=(me, (core + j) % tp), device_id_type=MESH,
        )
        for j in range(1, tp)
    ]

    @pl.when(core == holder)
    def _():
        for i in range(n):
            pltpu.make_async_copy(xr.at[i], xr.at[i], x_recv.at[i]).wait()
        for copy in handed:
            copy.start()

    for j in range(1, tp):

        @pl.when((holder + j) % tp == core)
        def _(j=j):
            handed[j - 1].wait_recv()

    inputs = permuted(
        xr[...].reshape(n * rows_each, features),
        lambda r: (r % (n * block_rows)) // block_rows * rows_each
        + r // (n * block_rows) * block_rows + r % block_rows,
    )
    group_rows = n * block_rows
    forwards, first_copies, second_copies = [], [], []
    pair, bit = z // 2, z % 2
    mate = pair * 2 + 1 - bit

    def partial_copy(c, slot, source, target_ref, to):
        copy = pltpu.make_async_remote_copy(
            src_ref=source, dst_ref=target_ref,
            send_sem=r_send.at[c, slot], recv_sem=r_recv.at[c, slot],
            device_id=(to * plane + p, core), device_id_type=MESH,
        )
        copy.start()
        return copy

    def own_rows(c, owner):
        return pf[c, owner]

    def received(c):
        return (pa_k, sb_k, pb_k) if c < per_matrix else (pa_v, sb_v, pb_v)

    def multiply(c):
        await_corner(c)
        product = jnp.dot(inputs, w[c].reshape(plane * w.shape[2], chunk), preferred_element_type=F32)
        pf[c] = product.reshape(depth, group_rows, chunk)
        sums = pf
        if c >= per_matrix:
            ps[c] = product.astype(BF16).reshape(depth, group_rows, chunk)
            sums = ps
        pa = received(c)[0]
        copies = []
        for o in list(range(1, pairs)) + [0]:
            owner = (pair + o) % pairs * 2 + 1 - bit
            copies.append(partial_copy(c, o, sums.at[c, owner], pa.at[c, o], mate))
        first_copies.append(copies)

    def pass_on(c):
        copies = []
        pa, sb, pb = received(c)
        for index, o in enumerate(range(1, pairs)):
            owner = (pair + o) % pairs * 2 + bit
            first_copies[c][index].wait_recv()
            sb[c, o] = (own_rows(c, owner) + pa[c, o].astype(F32)).astype(sb.dtype)
            copies.append(partial_copy(c, pairs + o, sb.at[c, o], pb.at[c, o], owner))
        second_copies.append(copies)

    def finish(c):
        first_copies[c][pairs - 1].wait_recv()
        pa, _, pb = received(c)
        total = own_rows(c, z) + pa[c, 0].astype(F32)
        for o in range(1, pairs):
            second_copies[c][o - 1].wait_recv()
            total = total + pb[c, o].astype(F32)
        base = (c % per_matrix) * chunk
        block = kb if c < per_matrix else vb
        block[:, base : base + chunk] = total.astype(BF16)

    for c in range(CHUNKS):
        forwards.append(forward_weights(c))
        if c + 2 < CHUNKS:
            weight_copies.append(send_weights(c + 2))
        if c == CHUNKS - 1:
            key_copies = distribute(0, key_bundles, tk, pk)
            value_copies = distribute(1, value_bundles, tv, pv)
        if c >= 1:
            multiply(c - 1)
        if c >= 2:
            pass_on(c - 2)
        if c >= 3:
            finish(c - 3)
    multiply(CHUNKS - 1)
    pass_on(CHUNKS - 2)
    finish(CHUNKS - 3)

    for copy in gate_copies:
        copy.wait_recv()
    gates = jnp.zeros((heads, lanes), F32)
    blocks = [jnp.zeros((heads, lanes), F32) for _ in range(pl.cdiv(n * per, lanes))]
    for i in range(n):
        shift = (i * block_rows - past_rows) % lanes
        moved = pltpu.roll(gr[i], shift, 1) if shift else gr[i]
        gates = jnp.where(lane // block_rows == i, moved, gates)
        shift = i * per % lanes
        moved = pltpu.roll(gr[i], shift, 1) if shift else gr[i]
        for number in range(len(blocks)):
            blocks[number] = jnp.where((lane + number * lanes) // per == i, moved, blocks[number])
    for number, values in enumerate(blocks):
        low, high = number * lanes, min((number + 1) * lanes, n * per)
        cg_ref[:, low:high] = values[:, : high - low]

    pass_on(CHUNKS - 1)
    finish(CHUNKS - 2)

    def assembled(past, block):
        rows = jnp.concatenate([past.reshape(n * past_rows, width), block], axis=0)

        def row_source(r):
            source, place = r // per, r % per
            return jnp.where(
                place < past_rows,
                source * past_rows + place,
                n * past_rows + source * block_rows + place - past_rows,
            )

        return permuted(rows, row_source)

    for copy in key_copies:
        copy.wait_recv()
    ck_ref[...] = assembled(pk[...], kb[...])
    own_score = jnp.sum(query * own_key, axis=1, keepdims=True) * head_width ** (-0.5)
    finish(CHUNKS - 1)

    read = merge_pair(
        read,
        block_read(query_diagonal, kb[...], vb[...], gates[:, :group_rows], gate_here, heads),
    )
    half = head_width // 2
    _, lane = iotas(heads, head_width)
    st[0:heads, :] = jnp.where(lane < half, read[0], read[1])
    st[heads : 2 * heads, :] = read[2]
    stat_copies = []
    for k in range(1, n):
        copy = pltpu.make_async_remote_copy(
            src_ref=st, dst_ref=sr.at[k],
            send_sem=s_send.at[k], recv_sem=s_recv.at[k],
            device_id=((me + k) % n, core), device_id_type=MESH,
        )
        copy.start()
        stat_copies.append(copy)

    for copy in value_copies:
        copy.wait_recv()
    cv_ref[...] = assembled(pv[...], vb[...])

    read = merge_pair(read, (own_score, jnp.ones_like(own_score), own_value))
    for copy in stat_copies:
        copy.wait_recv()
    for k in range(1, n):
        read = merge_pair(
            read, (sr[k, 0:heads, 0:1], sr[k, 0:heads, half : half + 1], sr[k, heads : 2 * heads, :])
        )
    result = read[2] / read[1]
    for head in range(heads):
        out_ref[:, head * head_width : (head + 1) * head_width] = result[head : head + 1, :]

    for zz in range(z_each):
        for q in range(plane):
            target, remote, _ = input_copy(zz, q)

            @pl.when(target != me)
            def _(remote=remote):
                remote.wait_send()

    @pl.when(core == holder)
    def _():
        for copy in handed:
            copy.wait_send()

    for copies in (
        weight_copies + forwards + first_copies + second_copies
        + [gate_copies, key_bundles, value_bundles, key_copies, value_copies, stat_copies]
    ):
        for copy in copies:
            copy.wait_send()


def fused(
    n, tp, plane,
    block_input, key_weight, value_weight, earlier_keys, past_values, past_gates, block_gates,
    step_query, step_key, step_value, step_gate,
):
    span, features_here = block_input.shape[1:]
    kept, width = key_weight.shape
    heads = width // HEAD_DIM
    past_rows = earlier_keys.shape[1] // n
    block_rows = span // n
    depth = n // plane
    per = past_rows + block_rows
    lanes = HEAD_DIM
    chunk = 2 * width // CHUNKS
    group_rows = n * block_rows
    dims = (span, past_rows, block_rows, width, heads)
    vmem = pl.BlockSpec(memory_space=pltpu.VMEM)
    hbm = pl.BlockSpec(memory_space=pltpu.HBM)
    dma = pltpu.SemaphoreType.DMA
    rows = pltpu.VMEM((depth, plane, past_rows, width), BF16)
    wide = pltpu.VMEM((CHUNKS, depth // 2, group_rows, chunk), F32)
    partials = pltpu.VMEM((CHUNKS, depth // 2, group_rows, chunk), BF16)
    keys, values, gates, read = pl.pallas_call(
        functools.partial(kernel, n, tp, plane, dims),
        name="relay",
        out_shape=(
            jax.ShapeDtypeStruct((n * per, width), BF16),
            jax.ShapeDtypeStruct((n * per, width), BF16),
            jax.ShapeDtypeStruct((heads, n * per), F32),
            jax.ShapeDtypeStruct((1, width), F32),
        ),
        in_specs=[hbm] * 5 + [vmem] * 6,
        out_specs=(vmem,) * 4,
        scratch_shapes=[
            pltpu.VMEM((span, features_here), BF16),
            rows,
            rows,
            pltpu.VMEM((n, heads, lanes), F32),
            pltpu.VMEM((span, features_here), BF16),
            pltpu.VMEM((n, depth * block_rows, plane * kept), BF16),
            pltpu.VMEM((CHUNKS, plane, kept, chunk), BF16),
            pltpu.VMEM((CHUNKS, depth, group_rows, chunk), F32),
            pltpu.VMEM((CHUNKS, depth, group_rows, chunk), BF16),
            wide,
            wide,
            wide,
            partials,
            partials,
            partials,
            rows,
            rows,
            rows,
            rows,
            pltpu.VMEM((n, heads, lanes), F32),
            pltpu.VMEM((2 * heads, HEAD_DIM), F32),
            pltpu.VMEM((n, 2 * heads, HEAD_DIM), F32),
            pltpu.VMEM((group_rows, width), BF16),
            pltpu.VMEM((group_rows, width), BF16),
            dma((3 + CHUNKS,)),
            dma((depth // tp * plane,)),
            dma((n,)),
            dma((tp,)),
            dma((tp,)),
            dma((CHUNKS, 4)),
            dma((CHUNKS, 4)),
            dma((2, depth)),
            dma((2, depth)),
            dma((3, n)),
            dma((3, n)),
            dma((CHUNKS, depth)),
            dma((CHUNKS, depth)),
            dma((n,)),
            dma((n,)),
        ],
        compiler_params=pltpu.CompilerParams(
            collective_id=0, has_side_effects=True, vmem_limit_bytes=48 * 1024 * 1024
        ),
    )(
        block_input[0],
        key_weight,
        value_weight,
        earlier_keys.reshape(depth, plane, past_rows, width),
        past_values.reshape(depth, plane, past_rows, width),
        past_gates[0],
        block_gates[0],
        step_query,
        step_key,
        step_value,
        step_gate,
    )
    return keys[None], values[None], gates[None], read


def plane_size(n):
    plane = 1
    while 4 * plane * plane <= n:
        plane *= 2
    return plane


def fits(n, tp, args):
    block_input, key_weight, earlier_keys = args[0], args[1], args[3]
    plane = plane_size(n)
    depth = n // plane
    span, width = block_input.shape[1], key_weight.shape[1]
    heads = width // HEAD_DIM
    past_rows, block_rows = earlier_keys.shape[1] // n, span // n
    return (
        block_input.shape[0] == 1 and n == GROUP and plane == 4 and n % plane == 0 and depth % (2 * tp) == 0
        and span % n == 0 and past_rows % 16 == 0 and (depth * block_rows) % 16 == 0
        and HEAD_DIM % past_rows == 0 and past_rows + block_rows <= HEAD_DIM
        and HEAD_DIM % span == 0
        and heads % 8 == 0 and width % (CHUNKS // 2 * HEAD_DIM) == 0
    )


def local_program(n, tp, *args):
    if fits(n, tp, args):
        return fused(n, tp, plane_size(n), *args)
    return local(*args)


def solution(mesh):
    in_specs = (
        P(None, "sp", "tp"),
        P("sp", "tp"),
        P("sp", "tp"),
        P(None, "sp", "tp"),
        P(None, "sp", "tp"),
        P(None, "tp", "sp"),
        P(None, "tp", "sp"),
        P(None, "tp"),
        P(None, "tp"),
        P(None, "tp"),
        P(None, "tp"),
    )
    out_specs = (P("sp", None, "tp"), P("sp", None, "tp"), P("sp", "tp", None), P(None, "tp"))
    body = functools.partial(local_program, mesh.shape["sp"], mesh.shape["tp"])
    return jax.shard_map(body, mesh=mesh, in_specs=in_specs, out_specs=out_specs, check_vma=False)
```
